32 devices in a mesh: fs: 8 (over z, x), tp: 4 (over y, core).
Axes of the slice: x: 2, y: 2, z: 4, core: 2. Of those that a mesh axis runs over, the one named last changes fastest.
Arguments:
- inputs: bfloat16 [8192, 4096], P('fs'), may hold values from -8 to 8
- value_cot: bfloat16 [8192, 2048], P('fs', 'tp'), may hold values from -0.015625 to 0.015625
- gate_cot: bfloat16 [8192, 2048], P('fs', 'tp'), may hold values from -0.015625 to 0.015625
- out_cot: bfloat16 [8192, 4096], P('fs'), may hold values from -0.0234375 to 0.0234375
- conv_output: bfloat16 [8192, 2048], P('fs', 'tp'), may hold values from -6 to 6
- factors: bfloat16 [3, 4096, 256], P(None, 'fs'), may hold values from -0.375 to 0.375
- value_weight: float32 [4096, 2048], P('fs', 'tp'), may hold values from -0.09375 to 0.09375
- gate_weight: float32 [4096, 2048], P('fs', 'tp'), may hold values from -0.09375 to 0.09375
- out_weight: float32 [2048, 4096], P('tp', 'fs'), may hold values from -0.125 to 0.125
- first_moment: float32 [3, 256, 2048], P(None, 'fs', 'tp'), may hold values from -7.2 to 7.2
- second_moment: float32 [3, 256, 2048], P(None, 'fs', 'tp'), may hold values from 0.005 to 0.05
Outputs:
- new_first: float32 [3, 256, 2048], P(None, 'fs', 'tp')
- new_second: float32 [3, 256, 2048], P(None, 'fs', 'tp')
- value_update: float32 [4096, 2048], P('fs', 'tp')
- gate_update: float32 [4096, 2048], P('fs', 'tp')
- out_update: float32 [2048, 4096], P('tp', 'fs')
- value_copy: bfloat16 [4096, 2048], P(None, 'tp')
- gate_copy: bfloat16 [4096, 2048], P(None, 'tp')
- out_copy: bfloat16 [2048, 4096], P('tp')
The draws below stay inside these ranges and needn't reach their ends.
All inputs are finite; a program needn't handle non-finite values.
Results may differ from the reference program's by a relative error of at most 0.001.
Values may be sent and summed in bfloat16 or wider, within the bound.
No kernel may reach another device: no remote copies, remote signals or barrier semaphores. Data moves between devices by JAX's collectives and lax.ppermute only.
A program may use at most 128 MiB of HBM per device.

```python
import math
import jax
import jax.numpy as jnp
from jax import lax

D = 4096
C = 2048
RANK = 256
TOKENS = 8192


def draw_first_moment(key, part):
    key_one, key_two = jax.random.split(jax.random.fold_in(key, 11), 2)
    row_rise = jnp.arange(RANK, dtype=jnp.float32) / max(RANK - 1, 1)
    col_rise = jnp.arange(C, dtype=jnp.float32) / max(C - 1, 1)
    rise_table = jnp.exp(jnp.log(3.0) * row_rise)[:, None] * jnp.exp(jnp.log(3.0) * col_rise)[None, :]
    roughness = jnp.exp(jax.random.uniform(key_two, (3, RANK, C), jnp.float32, 0.0, jnp.log(2.0)))
    base_draw = jnp.clip(jax.random.normal(key_one, (3, RANK, C), jnp.float32), -4.0, 4.0)
    return (0.1 * base_draw * rise_table[None, :, :] * roughness).astype(jnp.float32)


def spiked(result, rng, source, target, blocks, factor):
    owner, partner = [(jnp.arange(result.shape[axis_at]) // (result.shape[axis_at] // blocks)).reshape([-1 if axis == axis_at else 1 for axis in range(result.ndim)]) for axis_at in (source, target)]
    chosen = jax.random.permutation(rng, blocks)[partner]
    strong = (owner == chosen) | (owner == (partner + blocks // 2) % blocks)
    return jnp.where(strong, factor * result, result)


def block_levels(stream_key, extent, cuts, least, largest):
    factor_of = 1.0
    for dim, parts in cuts:
        draws = jax.random.uniform(jax.random.fold_in(jax.random.fold_in(stream_key, 6), dim), (parts,), jnp.float32, least / len(cuts), largest / len(cuts))
        factor_of = factor_of * jnp.repeat(jnp.exp(draws), extent[dim] // parts).reshape((-1,) + (1,) * (len(extent) - 1 - dim))
    return factor_of


def centred(own_key, dims, deviation, bound, cuts=(), held_as=jnp.bfloat16):
    result = deviation * jax.random.normal(own_key, dims, jnp.float32)
    if cuts:
        result = result * block_levels(own_key, dims, cuts, -0.22, 0.18)
    return jnp.clip(result, -bound, bound).astype(held_as)


def gaussian_with(key, extent, width, limit, pieces, heavy, kind=jnp.bfloat16):
    array = width * jax.random.normal(key, extent, jnp.float32)
    if pieces:
        array = array * block_levels(key, extent, pieces, -0.22, 0.18)
    return jnp.clip(spiked(array, jax.random.fold_in(key, 3), *heavy), -limit, limit).astype(kind)


def setup_inputs(seed: int = 0) -> dict:
    keys = jax.random.split(jax.random.key(seed), 12)
    inputs = gaussian_with(keys[0], (TOKENS, D), 1.0, 8.0, ((0, 8),), (0, 1, 8, 2.0))
    value_cot = centred(keys[1], (TOKENS, C), (RANK ** 0.5 * (D * TOKENS) ** -0.5), 0.015625, ((0, 8), (1, 4)))
    gate_cot = centred(keys[2], (TOKENS, C), (RANK ** 0.5 * (D * TOKENS) ** -0.5), 0.015625, ((0, 8), (1, 4)))
    out_cot = gaussian_with(keys[3], (TOKENS, D), (RANK ** 0.5 * (D * TOKENS) ** -0.5), 0.0234375, ((0, 8),), (0, 1, 8, 2.0))
    conv_output = centred(keys[4], (TOKENS, C), 1.0, 6.0, ((0, 8), (1, 4)))
    factors = centred(keys[5], (3, D, RANK), RANK ** -0.5, 0.375, ((1, 8),))
    value_weight = centred(keys[6], (D, C), D ** -0.5, 0.09375, ((0, 8), (1, 4)), jnp.float32)
    gate_weight = centred(keys[7], (D, C), D ** -0.5, 0.09375, ((0, 8), (1, 4)), jnp.float32)
    out_weight = centred(keys[8], (C, D), C ** -0.5, 0.125, ((0, 4), (1, 8)), jnp.float32)
    first_moment = draw_first_moment(jax.random.fold_in(keys[11], 71), 0)
    second_moment = jnp.clip(jnp.exp(math.log(0.05) - 2.3025851 * jax.random.uniform(keys[10], (3, RANK, C), jnp.float32) ** block_levels(keys[10], (3, RANK, C), ((1, 8), (2, 4)), -0.2, 0.2)), 0.005, 0.05)
    return dict(inputs=inputs, value_cot=value_cot, gate_cot=gate_cot, out_cot=out_cot, conv_output=conv_output, factors=factors, value_weight=value_weight, gate_weight=gate_weight, out_weight=out_weight, first_moment=first_moment, second_moment=second_moment)


FIRST_DECAY = 0.9
SECOND_DECAY = 0.95
DIVISOR_EPS = 1e-08
SQUARE_EPS = 1e-06
LEARN_RATE = 0.01

def project_side(source, factor, target):
    left_proj = jnp.dot(source.astype(jnp.float32), factor.astype(jnp.float32), precision=lax.Precision.HIGHEST)
    return jnp.dot(left_proj.T, target.astype(jnp.float32), precision=lax.Precision.HIGHEST)

def reference(inputs, value_cot, gate_cot, out_cot, conv_output, factors, value_weight, gate_weight, out_weight, first_moment, second_moment):
    projected = jnp.stack([project_side(inputs, factors[0], value_cot), project_side(inputs, factors[1], gate_cot), project_side(out_cot, factors[2], conv_output)])
    new_first = FIRST_DECAY * first_moment + (1.0 - FIRST_DECAY) * projected
    new_second = SECOND_DECAY * second_moment + (1.0 - SECOND_DECAY) * projected * projected
    direction = new_first / (jnp.sqrt(new_second) + DIVISOR_EPS)
    total = jnp.sum(direction * direction)
    norm_scale = lax.rsqrt(total / (3 * RANK * C) + SQUARE_EPS)
    float_factors = factors.astype(jnp.float32)
    value_update = norm_scale * jnp.dot(float_factors[0], direction[0], precision=lax.Precision.HIGHEST)
    gate_update = norm_scale * jnp.dot(float_factors[1], direction[1], precision=lax.Precision.HIGHEST)
    out_update = (norm_scale * jnp.dot(float_factors[2], direction[2], precision=lax.Precision.HIGHEST)).T
    value_copy = (value_weight - LEARN_RATE * value_update).astype(jnp.bfloat16)
    gate_copy = (gate_weight - LEARN_RATE * gate_update).astype(jnp.bfloat16)
    out_copy = (out_weight - LEARN_RATE * out_update).astype(jnp.bfloat16)
    return (new_first, new_second, value_update, gate_update, out_update, value_copy, gate_copy, out_copy)
```

```python
import math

import jax
import jax.numpy as jnp
from jax import lax
from jax.sharding import PartitionSpec as P

FIRST_DECAY = 0.9
SECOND_DECAY = 0.95
DIVISOR_EPS = 1e-08
SQUARE_EPS = 1e-06
LEARN_RATE = 0.01


def high_low(values):
    upper = lax.optimization_barrier(values.astype(jnp.bfloat16))
    lower = (values - upper.astype(jnp.float32)).astype(jnp.bfloat16)
    return (upper, lower)


def grid_sides(count):
    fast = max(side for side in range(1, math.isqrt(count) + 1) if count % side == 0)
    return count // fast, fast


def ring_order(count):
    slow, fast = grid_sides(count)
    if fast % 2 or slow < 2:
        return list(range(count))
    walk = []
    for column in range(fast):
        rows = range(1, slow) if column % 2 == 0 else range(slow - 1, 0, -1)
        walk += [row * fast + column for row in rows]
    return walk + [column for column in range(fast - 1, -1, -1)]


class Ring:
    def __init__(self, count):
        self.count = count
        self.order = ring_order(count)
        places = [0] * count
        for place, owner in enumerate(self.order):
            places[owner] = place
        self.place = jnp.array(places, jnp.int32)[lax.axis_index("fs")]
        self.owners = jnp.array(self.order, jnp.int32)
        self.ahead = [(self.order[i], self.order[(i + 1) % count]) for i in range(count)]
        self.behind = [(b, a) for a, b in self.ahead]

    def owner(self, offset):
        return self.owners[(self.place + offset) % self.count]

    def gather(self, piece, axis, split):
        extent = piece.shape[split]
        found = [(lax.axis_index("fs"), 0, piece)]
        forth = back = piece
        for step in range(1, (self.count - 1) // 2 + 1):
            forth = lax.ppermute(forth, "fs", self.ahead)
            back = lax.ppermute(back, "fs", self.behind)
            found.append((self.owner(-step), 0, forth))
            found.append((self.owner(step), 0, back))
        if self.count % 2 == 0:
            half = extent // 2
            first = lax.slice_in_dim(forth, 0, half, axis=split)
            second = lax.slice_in_dim(back, half, extent, axis=split)
            first = lax.ppermute(first, "fs", self.ahead)
            second = lax.ppermute(second, "fs", self.behind)
            far = self.owner(self.count // 2)
            found.append((far, 0, first))
            found.append((far, half, second))
        return found

    def whole(self, piece, axis, split):
        shape = list(piece.shape)
        size = shape[axis]
        shape[axis] = size * self.count
        out = jnp.zeros(tuple(shape), piece.dtype)
        for owner, start, part in self.gather(piece, axis, split):
            where = [0] * piece.ndim
            where[split] = start
            where[axis] = where[axis] + owner * size
            out = lax.dynamic_update_slice(out, part, where)
        return out


def pair_swap(values, axis_name, count, step):
    return lax.ppermute(values, axis_name, [(i, i ^ step) for i in range(count)])


def sum_everywhere(value, counts):
    for axis_name, count in counts:
        if count & (count - 1):
            value = lax.psum(value, axis_name)
            continue
        step = 1
        while step < count:
            value = value + pair_swap(value, axis_name, count, step)
            step *= 2
    return value


def exchange_add(parts, side, stride, count):
    place = (lax.axis_index("fs") // stride) % side
    take = lambda index: lax.dynamic_index_in_dim(parts, index, 0, keepdims=False)
    total = take(place)
    for shift in range(1, side):
        perm = []
        for device in range(count):
            at = (device // stride) % side
            perm.append((device, device + ((at + shift) % side - at) * stride))
        total = total + lax.ppermute(take((place + shift) % side), "fs", perm)
    return total


def reduce_rows(partial, count):
    slow, fast = grid_sides(count)
    rows, cols = partial.shape
    small = rows // count
    blocks = partial.reshape(slow, fast, small, cols).transpose(1, 0, 2, 3)
    kept = exchange_add(blocks, fast, 1, count)
    return exchange_add(kept, slow, fast, count)


def make_shards(fs_count, tp_count):
    def shards(
        inputs,
        value_cot,
        gate_cot,
        out_cot,
        conv_output,
        factors,
        value_weight,
        gate_weight,
        out_weight,
        first_moment,
        second_moment,
    ):
        ring = Ring(fs_count)
        rank = factors.shape[2]
        cols = value_cot.shape[1]
        entries = 3 * rank * cols * tp_count
        rows = factors.shape[1]
        if tp_count % 2 == 0:
            half = rows // 2
            side = lax.axis_index("tp") % 2
            mine = lax.dynamic_slice_in_dim(factors, side * half, half, axis=1)
            gathered = ring.whole(mine[:, None], 1, 2)
            other = pair_swap(gathered, "tp", tp_count, 1)
            low = jnp.where(side == 0, gathered, other)
            high = jnp.where(side == 0, other, gathered)
            pieces = jnp.concatenate([low, high], axis=2).reshape(3, rows * fs_count, rank)
        else:
            pieces = ring.whole(factors, 1, 1)
        sources = (inputs, inputs, out_cot)
        targets = (value_cot, gate_cot, conv_output)
        projected = []
        for index in range(3):
            summed = jnp.dot(sources[index], pieces[index], preferred_element_type=jnp.float32)
            upper, lower = high_low(summed)
            contract = lambda part: lax.dot_general(
                part,
                targets[index],
                (((0,), (0,)), ((), ())),
                preferred_element_type=jnp.float32,
            )
            projected.append(reduce_rows(contract(upper) + contract(lower), fs_count))
        projected = jnp.stack(projected)
        new_first = FIRST_DECAY * first_moment + (1.0 - FIRST_DECAY) * projected
        new_second = SECOND_DECAY * second_moment + (1.0 - SECOND_DECAY) * projected * projected
        direction = new_first / (jnp.sqrt(new_second) + DIVISOR_EPS)
        local = jnp.full((8, 128), jnp.sum(direction * direction), jnp.float32)
        total = sum_everywhere(local, (("tp", tp_count), ("fs", fs_count)))[:1, :1]
        norm_scale = lax.rsqrt(total / entries + SQUARE_EPS)
        collected = ring.whole(direction, 1, 2)
        updates = []
        for index in range(3):
            upper, lower = high_low(collected[index])
            if index < 2:
                product = lambda part: jnp.dot(
                    factors[index], part, preferred_element_type=jnp.float32
                )
            else:
                product = lambda part: lax.dot_general(
                    part,
                    factors[index],
                    (((0,), (1,)), ((), ())),
                    preferred_element_type=jnp.float32,
                )
            updates.append(norm_scale * (product(upper) + product(lower)))
        copies = []
        for index, weight in enumerate((value_weight, gate_weight, out_weight)):
            fresh = (weight - LEARN_RATE * updates[index]).astype(jnp.bfloat16)
            copies.append(ring.whole(fresh, 1 if index == 2 else 0, 0))
        return (new_first, new_second, *updates, *copies)

    return shards


def solution(mesh):
    placed = (
        P("fs", None),
        P("fs", "tp"),
        P("fs", "tp"),
        P("fs", None),
        P("fs", "tp"),
        P(None, "fs", None),
        P("fs", "tp"),
        P("fs", "tp"),
        P("tp", "fs"),
        P(None, "fs", "tp"),
        P(None, "fs", "tp"),
    )
    return jax.shard_map(
        make_shards(mesh.shape["fs"], mesh.shape["tp"]),
        mesh=mesh,
        in_specs=placed,
        out_specs=(
            P(None, "fs", "tp"),
            P(None, "fs", "tp"),
            P("fs", "tp"),
            P("fs", "tp"),
            P("tp", "fs"),
            P(None, "tp"),
            P(None, "tp"),
            P("tp", None),
        ),
        check_vma=False,
    )
```

```python
import math

import jax
import jax.numpy as jnp
from jax import lax
from jax.experimental.layout import Layout, with_layout_constraint
from jax.sharding import PartitionSpec as P

FIRST_DECAY = 0.9
SECOND_DECAY = 0.95
DIVISOR_EPS = 1e-08
SQUARE_EPS = 1e-06
LEARN_RATE = 0.01


def high_low(values):
    upper = lax.optimization_barrier(values.astype(jnp.bfloat16))
    lower = (values - upper.astype(jnp.float32)).astype(jnp.bfloat16)
    return (upper, lower)


def grid_sides(count):
    fast = max(side for side in range(1, math.isqrt(count) + 1) if count % side == 0)
    return count // fast, fast


def ring_order(count):
    slow, fast = grid_sides(count)
    if fast % 2 or slow < 2:
        return list(range(count))
    walk = []
    for column in range(fast):
        rows = range(1, slow) if column % 2 == 0 else range(slow - 1, 0, -1)
        walk += [row * fast + column for row in rows]
    return walk + [column for column in range(fast - 1, -1, -1)]


class Ring:
    def __init__(self, count):
        self.count = count
        self.order = ring_order(count)
        places = [0] * count
        for place, owner in enumerate(self.order):
            places[owner] = place
        self.place = jnp.array(places, jnp.int32)[lax.axis_index("fs")]
        self.owners = jnp.array(self.order, jnp.int32)
        self.ahead = [(self.order[i], self.order[(i + 1) % count]) for i in range(count)]
        self.behind = [(b, a) for a, b in self.ahead]

    def owner(self, offset):
        return self.owners[(self.place + offset) % self.count]

    def gather(self, piece, axis, split):
        extent = piece.shape[split]
        found = [(lax.axis_index("fs"), 0, piece)]
        forth = back = piece
        for step in range(1, (self.count - 1) // 2 + 1):
            forth = lax.ppermute(forth, "fs", self.ahead)
            back = lax.ppermute(back, "fs", self.behind)
            found.append((self.owner(-step), 0, forth))
            found.append((self.owner(step), 0, back))
        if self.count % 2 == 0:
            half = extent // 2
            first = lax.slice_in_dim(forth, 0, half, axis=split)
            second = lax.slice_in_dim(back, half, extent, axis=split)
            first = lax.ppermute(first, "fs", self.ahead)
            second = lax.ppermute(second, "fs", self.behind)
            far = self.owner(self.count // 2)
            found.append((far, 0, first))
            found.append((far, half, second))
        return found

    def whole(self, piece, axis, split):
        shape = list(piece.shape)
        size = shape[axis]
        shape[axis] = size * self.count
        out = jnp.zeros(tuple(shape), piece.dtype)
        found = self.gather(piece, axis, split)
        for owner, start, part in found[1:3] + found[:1] + found[3:]:
            where = [0] * piece.ndim
            where[split] = start
            where[axis] = where[axis] + owner * size
            out = lax.dynamic_update_slice(out, part, where)
        return out


def pair_swap(values, axis_name, count, step):
    return lax.ppermute(values, axis_name, [(i, i ^ step) for i in range(count)])


def sum_everywhere(value, counts):
    for axis_name, count in counts:
        if count & (count - 1):
            value = lax.psum(value, axis_name)
            continue
        step = 1
        while step < count:
            value = value + pair_swap(value, axis_name, count, step)
            step *= 2
    return value


def exchange_add(parts, side, stride, count):
    place = (lax.axis_index("fs") // stride) % side
    take = lambda index: lax.dynamic_index_in_dim(parts, index, 0, keepdims=False)
    total = take(place)
    for shift in range(1, side):
        perm = []
        for device in range(count):
            at = (device // stride) % side
            perm.append((device, device + ((at + shift) % side - at) * stride))
        total = total + lax.ppermute(take((place + shift) % side), "fs", perm)
    return total


def reduce_rows(partial, count):
    slow, fast = grid_sides(count)
    rows, cols = partial.shape
    small = rows // count
    blocks = partial.reshape(slow, fast, small, cols).transpose(1, 0, 2, 3)
    kept = exchange_add(blocks, fast, 1, count)
    return exchange_add(kept, slow, fast, count)


def pinned(values):
    return with_layout_constraint(values, Layout((0, 1)))


def make_shards(fs_count, tp_count):
    def shards(
        inputs,
        value_cot,
        gate_cot,
        out_cot,
        conv_output,
        factors,
        value_weight,
        gate_weight,
        out_weight,
        first_moment,
        second_moment,
    ):
        ring = Ring(fs_count)
        rank = factors.shape[2]
        cols = value_cot.shape[1]
        entries = 3 * rank * cols * tp_count
        rows = factors.shape[1]
        if tp_count % 2 == 0:
            half = rows // 2
            side = lax.axis_index("tp") % 2
            mine = lax.dynamic_slice_in_dim(factors, side * half, half, axis=1)
            gathered = ring.whole(mine[:, None], 1, 2)
            other = pair_swap(gathered, "tp", tp_count, 1)
            both = jnp.zeros((3, fs_count, 2, half, rank), factors.dtype)
            both = lax.dynamic_update_slice(both, gathered[:, :, None], (0, 0, side, 0, 0))
            both = lax.dynamic_update_slice(both, other[:, :, None], (0, 0, 1 - side, 0, 0))
            pieces = both.reshape(3, rows * fs_count, rank)
        else:
            pieces = ring.whole(factors, 1, 1)
        sources = (inputs, inputs, out_cot)
        targets = (value_cot, gate_cot, conv_output)
        projected = []
        for index in range(3):
            summed = jnp.dot(sources[index], pieces[index], preferred_element_type=jnp.float32)
            upper, lower = high_low(summed)
            contract = lambda part: lax.dot_general(
                part,
                targets[index],
                (((0,), (0,)), ((), ())),
                preferred_element_type=jnp.float32,
            )
            projected.append(reduce_rows(contract(upper) + contract(lower), fs_count))
        projected = jnp.stack(projected)
        new_first = FIRST_DECAY * first_moment + (1.0 - FIRST_DECAY) * projected
        new_second = SECOND_DECAY * second_moment + (1.0 - SECOND_DECAY) * projected * projected
        direction = new_first / (jnp.sqrt(new_second) + DIVISOR_EPS)
        local = jnp.full((8, 128), jnp.sum(direction * direction), jnp.float32)
        total = sum_everywhere(local, (("tp", tp_count), ("fs", fs_count)))[:1, :1]
        norm_scale = lax.rsqrt(total / entries + SQUARE_EPS)
        collected = ring.whole(direction, 1, 2)
        updates = []
        for index in range(3):
            upper, lower = high_low(collected[index])
            if index < 2:
                product = lambda part: jnp.dot(
                    factors[index], part, preferred_element_type=jnp.float32
                )
            else:
                product = lambda part: lax.dot_general(
                    part,
                    factors[index],
                    (((0,), (1,)), ((), ())),
                    preferred_element_type=jnp.float32,
                )
            updates.append(pinned(norm_scale * (product(upper) + product(lower))))
        copies = []
        for index, weight in enumerate((value_weight, gate_weight, out_weight)):
            fresh = pinned((weight - LEARN_RATE * updates[index]).astype(jnp.bfloat16))
            copies.append(ring.whole(fresh, 1 if index == 2 else 0, 0))
        return (new_first, new_second, *updates, *copies)

    return shards


def solution(mesh):
    placed = (
        P("fs", None),
        P("fs", "tp"),
        P("fs", "tp"),
        P("fs", None),
        P("fs", "tp"),
        P(None, "fs", None),
        P("fs", "tp"),
        P("fs", "tp"),
        P("tp", "fs"),
        P(None, "fs", "tp"),
        P(None, "fs", "tp"),
    )
    return jax.shard_map(
        make_shards(mesh.shape["fs"], mesh.shape["tp"]),
        mesh=mesh,
        in_specs=placed,
        out_specs=(
            P(None, "fs", "tp"),
            P(None, "fs", "tp"),
            P("fs", "tp"),
            P("fs", "tp"),
            P("tp", "fs"),
            P(None, "tp"),
            P(None, "tp"),
            P("tp", None),
        ),
        check_vma=False,
    )
```
